128 devices in a mesh: ep: 32 (over z, y, core), tp: 4 (over x).
Axes of the slice: x: 4, y: 4, z: 4, core: 2. Of those that a mesh axis runs over, the one named last changes fastest.
Arguments:
- query_rows: bfloat16 [16384, 1024], P('ep', 'tp'), may hold values from -60 to 60
- key_rows: bfloat16 [16384, 1024], P('ep', 'tp'), may hold values from -6 to 6
- value_rows: bfloat16 [16384, 1024], P('ep', 'tp'), may hold values from -6 to 6
- lambdas: float32 [8], P('tp'), may hold values from 0.3 to 0.8
- out_gain: float32 [128], replicated, may hold values from 0.1 to 1.9
- out_weight: bfloat16 [1024, 2048], P('tp'), may hold values from -0.1875 to 0.1875
- tokens: bfloat16 [16384, 2048], P(('ep', 'tp')), may hold values from -6 to 6
- norm_gain: float32 [2048], replicated, may hold values from 0.1 to 1.9
- group_ids: int32 [16384], P(('ep', 'tp')), may hold values from 0 to 3, as said below
- inner_ids: int32 [16384, 2], P(('ep', 'tp')), may hold values from 0 to 7, as said below
- route_weights: float32 [16384, 2], P(('ep', 'tp')), may hold values from 0.2 to 1
- gate_weight: bfloat16 [32, 2048, 1024], P('ep', None, 'tp'), may hold values from -0.125 to 0.125
- up_weight: bfloat16 [32, 2048, 1024], P('ep', None, 'tp'), may hold values from -0.125 to 0.125
- down_weight: bfloat16 [32, 1024, 2048], P('ep', 'tp'), may hold values from -0.1875 to 0.1875
Outputs:
- attended: bfloat16 [16384, 2048], P(('ep', 'tp'))
- combined: bfloat16 [16384, 2048], P(('ep', 'tp'))
The draws below stay inside these ranges and needn't reach their ends.
Inputs may be any that keep to these rules, and one draw needn't show every extreme that they name: In the 128 rows of one device no expert group_ids * 8 + inner_ids is named more than 10 times; some expert is named exactly 10 times in the rows of every device. `inner_ids`: the 2 entries of a row are different.
All inputs are finite; a program needn't handle non-finite values.
Results may differ from the reference program's by a relative error of at most 0.013.
Values may be sent and summed in bfloat16 or wider, within the bound.
A program may use at most 128 MiB of HBM per device.

```python
import jax
import jax.numpy as jnp
from jax import lax

D = 2048
HEADS = 8
DQ = 64
DV = 128
FF = 1024
GROUPS = 4
TOPK = 2
TOK_DEV = 128
SEG = 512
TOKENS = 16384
EXPERTS = 32
CAP = 10
N_EP = 32
N_TP = 4


def paired_scores(base_key):
    width_cols = HEADS * 2 * DQ
    query_base = jnp.clip(jax.random.normal(jax.random.fold_in(base_key, 21), (TOKENS, width_cols), jnp.float32), -4.5, 4.5) * 1.3
    key_base = jnp.clip(jax.random.normal(jax.random.fold_in(base_key, 22), (TOKENS, width_cols), jnp.float32), -4.5, 4.5) * 1.3
    return (query_base, key_base)


def draw_query_rows(key, part):
    return paired_scores(key)[0].astype(jnp.bfloat16)


def draw_key_rows(key, part):
    return paired_scores(key)[1].astype(jnp.bfloat16)


def route_cells(base_key):
    group_size = EXPERTS // GROUPS
    per_row = group_size // TOPK
    per_group = CAP * per_row
    blocks = TOKENS // TOK_DEV
    hot = jax.random.randint(jax.random.fold_in(base_key, 31), (), 0, GROUPS).astype(jnp.int32)

    def one_block(block_num):
        block_key = jax.random.fold_in(jax.random.fold_in(base_key, 32), block_num)
        spare = jax.random.permutation(jax.random.fold_in(block_key, 1), (GROUPS - 1) * per_group)
        spare = spare[:TOK_DEV - per_group].astype(jnp.int32)
        spare_group = spare // per_group
        spare_group = spare_group + (spare_group >= hot).astype(jnp.int32)
        cell_group = jnp.concatenate([jnp.zeros((per_group,), jnp.int32) + hot, spare_group])
        cell_local = jnp.concatenate([jnp.arange(per_group, dtype=jnp.int32), spare % per_group])
        order = jax.random.permutation(jax.random.fold_in(block_key, 2), TOK_DEV).astype(jnp.int32)
        tok_group = cell_group[order]
        tok_local = cell_local[order]
        row_of = tok_group * CAP + tok_local // per_row
        slot_num = tok_local % per_row
        scores = jax.random.randint(jax.random.fold_in(block_key, 3), (GROUPS * CAP, group_size), 0, 1 << 20)
        scores = scores * group_size + jnp.arange(group_size, dtype=jnp.int32)[None, :]
        shuffle = jnp.argsort(scores, axis=1).astype(jnp.int32)
        columns = slot_num[:, None] * TOPK + jnp.arange(TOPK, dtype=jnp.int32)[None, :]
        chosen = jnp.take_along_axis(shuffle[row_of], columns, axis=1)
        return (tok_group, chosen)
    groups_all, inner_all = jax.vmap(one_block)(jnp.arange(blocks, dtype=jnp.int32))
    return (groups_all.reshape(TOKENS).astype(jnp.int32), inner_all.reshape(TOKENS, TOPK).astype(jnp.int32))


def draw_group_ids(key, part):
    return route_cells(key)[0]


def draw_inner_ids(key, part):
    return route_cells(key)[1]


def level_of(stream_key, shape, split, least, top_value):
    level, own = 1.0, jax.random.fold_in(stream_key, 6)
    for axis_at, parts in split:
        draws = jnp.exp(jax.random.uniform(jax.random.fold_in(own, axis_at), (parts,), jnp.float32, least / len(split), top_value / len(split)))
        level = level * jnp.repeat(draws, shape[axis_at] // parts).reshape([-1 if axis == axis_at else 1 for axis in range(len(shape))])
    return level


def normal_values(stream_key, extent, scale, bound, cuts=(), kind=jnp.bfloat16):
    values = jax.random.normal(stream_key, extent, jnp.float32) * scale
    if len(cuts) > 0:
        values = level_of(stream_key, extent, cuts, -0.22, 0.18) * values
    return jnp.clip(values, min=-bound, max=bound).astype(kind)


def setup_inputs(seed: int = 0) -> dict:
    keys = jax.random.split(jax.random.key(seed), 15)
    query_rows = draw_query_rows(jax.random.fold_in(keys[14], 71), 0)
    key_rows = draw_key_rows(jax.random.fold_in(keys[14], 71), 0)
    value_rows = normal_values(keys[2], (TOKENS, HEADS * DV), 1.0, 6.0, ((0, 32), (1, 4)))
    lambdas = jnp.clip(0.3 + 0.5 * jax.random.uniform(keys[3], (HEADS,), jnp.float32) ** level_of(keys[3], (HEADS,), ((0, 4),), -0.2, 0.2), 0.3, 0.8)
    out_gain = jnp.clip(1.0 + 0.18 * jax.random.normal(keys[4], (DV,), jnp.float32), 0.1, 1.9)
    out_weight = normal_values(keys[5], (HEADS * DV, D), (HEADS * DV) ** -0.5, 0.1875, ((0, 4),))
    tokens = normal_values(keys[6], (TOKENS, D), 1.0, 6.0, ((0, 128),))
    norm_gain = jnp.clip(1.0 + 0.18 * jax.random.normal(keys[7], (D,), jnp.float32), 0.1, 1.9)
    group_ids = draw_group_ids(jax.random.fold_in(keys[14], 71), 0)
    inner_ids = draw_inner_ids(jax.random.fold_in(keys[14], 71), 0)
    route_weights = jnp.clip(0.2 + 0.8 * jax.random.uniform(keys[10], (TOKENS, TOPK), jnp.float32) ** level_of(keys[10], (TOKENS, TOPK), ((0, 128),), -0.2, 0.2), 0.2, 1.0)
    gate_weight = normal_values(keys[11], (EXPERTS, D, FF), D ** -0.5, 0.125, ((0, 32), (2, 4)))
    up_weight = normal_values(keys[12], (EXPERTS, D, FF), D ** -0.5, 0.125, ((0, 32), (2, 4)))
    down_weight = normal_values(keys[13], (EXPERTS, FF, D), FF ** -0.5, 0.1875, ((0, 32), (1, 4)))
    return dict(query_rows=query_rows, key_rows=key_rows, value_rows=value_rows, lambdas=lambdas, out_gain=out_gain, out_weight=out_weight, tokens=tokens, norm_gain=norm_gain, group_ids=group_ids, inner_ids=inner_ids, route_weights=route_weights, gate_weight=gate_weight, up_weight=up_weight, down_weight=down_weight)


eps = 1e-06

def one_map(query_part, key_all, value_all, allowed):
    scores = jnp.dot(query_part, key_all.T, preferred_element_type=jnp.float32) * DQ ** (-0.5)
    scores = jnp.where(allowed, scores, -jnp.inf)
    row_top = lax.optimization_barrier(jnp.max(scores, axis=1, keepdims=True))
    exps = jnp.exp(scores - row_top)
    totals = lax.optimization_barrier(jnp.sum(exps, axis=1, keepdims=True))
    weighted = jnp.dot(exps.astype(jnp.bfloat16), value_all, preferred_element_type=jnp.float32)
    return weighted / totals

def head_output(operands):
    query_head, key_head, value_head, lambda_head = operands
    key_pos = jnp.arange(TOKENS, dtype=jnp.int32)

    def query_block(block_num):
        first_row = block_num * SEG
        query_part = lax.dynamic_slice_in_dim(query_head, first_row, SEG, 0)
        query_pos = first_row + jnp.arange(SEG, dtype=jnp.int32)
        allowed = key_pos[None, :] <= query_pos[:, None]
        first_map = one_map(query_part[:, 0], key_head[:, 0], value_head, allowed)
        second_map = one_map(query_part[:, 1], key_head[:, 1], value_head, allowed)
        heads_out = first_map - lambda_head * second_map
        mean_sq = lax.optimization_barrier(jnp.mean(heads_out * heads_out, axis=1, keepdims=True))
        return heads_out * lax.rsqrt(mean_sq + eps)
    return lax.map(query_block, jnp.arange(N_EP, dtype=jnp.int32)).reshape(TOKENS, DV)

def reference(query_rows, key_rows, value_rows, lambdas, out_gain, out_weight, tokens, norm_gain, group_ids, inner_ids, route_weights, gate_weight, up_weight, down_weight):
    query_heads = query_rows.reshape(TOKENS, HEADS, 2, DQ).transpose(1, 0, 2, 3)
    key_heads = key_rows.reshape(TOKENS, HEADS, 2, DQ).transpose(1, 0, 2, 3)
    value_heads = value_rows.reshape(TOKENS, HEADS, DV).transpose(1, 0, 2)
    per_head = lax.map(head_output, (query_heads, key_heads, value_heads, lambdas))
    normed_heads = (per_head * out_gain).astype(jnp.bfloat16).transpose(1, 0, 2).reshape(TOKENS, HEADS * DV)
    attended = jnp.dot(normed_heads, out_weight, preferred_element_type=jnp.float32).astype(jnp.bfloat16)
    tok_wide = tokens.astype(jnp.float32)
    normed = (tok_wide * lax.rsqrt(lax.optimization_barrier(jnp.mean(tok_wide * tok_wide, axis=1, keepdims=True)) + eps) * norm_gain).astype(jnp.bfloat16)
    picks = (group_ids[:, None] * (EXPERTS // GROUPS) + inner_ids).reshape(-1)
    flat_weights = route_weights.reshape(-1)
    room = N_EP * N_TP * CAP

    def one_expert(running, expert_num):
        matches = picks == expert_num
        picked = jnp.nonzero(matches, size=room, fill_value=0)[0].astype(jnp.int32)
        live = jnp.arange(room) < jnp.sum(matches)
        token_ids = picked // TOPK
        chosen_rows = normed[token_ids]
        gate_pre = jnp.dot(chosen_rows, gate_weight[expert_num], preferred_element_type=jnp.float32)
        up_pre = jnp.dot(chosen_rows, up_weight[expert_num], preferred_element_type=jnp.float32)
        hidden = (jax.nn.silu(gate_pre) * up_pre).astype(jnp.bfloat16)
        result = jnp.dot(hidden, down_weight[expert_num], preferred_element_type=jnp.float32).astype(jnp.bfloat16)
        weight_col = jnp.where(live, flat_weights[picked], jnp.float32(0.0))
        running = running.at[token_ids].add(result.astype(jnp.float32) * weight_col[:, None])
        return (running, None)
    running, _ = lax.scan(one_expert, jnp.zeros((TOKENS, D), jnp.float32), jnp.arange(EXPERTS, dtype=jnp.int32))
    combined = running.astype(jnp.bfloat16)
    return (attended, combined)
```

```python
import functools
import math

import jax
import jax.numpy as jnp
from jax import lax
from jax.experimental import pallas as pl
from jax.experimental.pallas import tpu as pltpu
from jax.sharding import PartitionSpec as P

GROUPS = 4
SIDE = 4
CHIPS = 16
MESH = pl.DeviceIdType.MESH

eps = 1e-06
neg_big = -1e30
f32 = jnp.float32
bf16 = jnp.bfloat16


def wrap(v):
    return lax.rem(v + SIDE, SIDE)


def attention_kernel(
    q_ref,
    k_ref,
    v_ref,
    lam_ref,
    gain_ref,
    ow_ref,
    out_ref,
    kv,
    give,
    qb,
    qt,
    acc,
    top,
    tot,
    ow,
    heads,
    outgoing,
    pre_send,
    pre_recv,
    here,
    kv_send,
    kv_recv,
    ow_send,
    ow_recv,
    head_send,
    head_recv,
):
    ep = lax.axis_index("ep")
    x = lax.axis_index("tp")
    chip = ep // 2
    core = lax.rem(ep, 2)
    mate = 1 - core
    mirror = CHIPS - 1 - chip
    at_z, at_y = chip // SIDE, lax.rem(chip, SIDE)
    right, left, far = wrap(x + 1), wrap(x - 1), wrap(x + 2)
    scale = (64 ** (-0.5)) * math.log2(math.e)

    def remote(src, dst, send, recv, to):
        return pltpu.make_async_remote_copy(
            src_ref=src, dst_ref=dst, send_sem=send, recv_sem=recv, device_id=to, device_id_type=MESH
        )

    def cols(head):
        return pl.ds(pl.multiple_of(head * 128, 128), 128)

    def chip_at(dz, dy):
        return wrap(at_z + dz) * SIDE + wrap(at_y + dy)

    partner = (2 * chip + mate, x)

    keep_q = pltpu.make_async_copy(q_ref.at[:, cols(0)], qb.at[0], here.at[0])
    give_q = remote(q_ref.at[:, cols(1)], qb.at[0], pre_send.at[1], pre_recv.at[1], partner)
    far_q = [
        remote(q_ref.at[:, cols(h)], qb.at[1], pre_send.at[1 + h], pre_recv.at[2], (2 * mirror + h, x))
        for h in range(2)
    ]

    @pl.when(core == 0)
    def _():
        keep_q.start()
        give_q.start()

    @pl.when(core == 1)
    def _():
        far_q[0].start()
        far_q[1].start()

    def lay_out(head, put):
        for p in range(2):
            put(p, pl.ds(0, 256), k_ref[pl.ds(p * 256, 256), cols(head)])
            for n in range(2):
                block = v_ref[pl.ds(p * 256 + n * 128, 128), cols(head)].astype(f32)
                put(p, pl.ds(256 + n * 128, 128), block.T.astype(bf16))

    def put_give(p, rows, value):
        give[p, rows, :] = value

    def put_own(p, rows, value):
        kv[chip, 2 * core + p, rows, :] = value

    lay_out(mate, put_give)
    half_of = kv.at[chip, pl.ds(2 * core, 2)]
    give_kv = remote(give, half_of, pre_send.at[0], pre_recv.at[0], partner)
    give_kv.start()
    lay_out(core, put_own)

    def step_to(axis, sign):
        return chip_at(sign, 0) if axis == 0 else chip_at(0, sign)

    def moved(place, axis, by):
        dz, dy = place
        return (dz + by, dy) if axis == 0 else (dz, dy + by)

    def spread(half, n, place, axis):
        def copy(slot):
            sign = 1 if slot % 2 == 0 else -1
            if slot < 2:
                j, part = chip_at(*place), pl.ds(2 * half, 2)
            else:
                j, part = chip_at(*moved(place, axis, -sign)), pl.ds(2 * half + slot - 2, 1)
            at = kv.at[j, part]
            return remote(
                at, at, kv_send.at[half, n, slot], kv_recv.at[half, n, slot], (2 * step_to(axis, sign) + core, x)
            )

        return [copy(slot) for slot in range(4)]

    first_axis = (1, 0)
    phase = [[None] * 5, [None] * 5]
    for half in range(2):
        one, two = first_axis[half], 1 - first_axis[half]
        phase[half][0] = spread(half, 0, (0, 0), one)
        for n, by in enumerate((0, -1, 1, 2)):
            phase[half][1 + n] = spread(half, 1 + n, moved((0, 0), one, by), two)
    sent = [c for half in range(2) for group in phase[half] for c in group]

    give_kv.wait_recv()
    for n in range(2):
        for half in range(2):
            phase[half][n][0].start()
            phase[half][n][1].start()

    keep_ow = pltpu.make_async_copy(ow_ref, ow.at[pl.ds(2 * x, 2)], here.at[1])
    keep_ow.start()

    def ow_rows(at_x, c):
        return ow.at[2 * at_x + c]

    ow_right = remote(ow_ref.at[core], ow_rows(x, core), ow_send.at[0], ow_recv.at[0], (ep, right))
    ow_left = remote(ow_ref.at[core], ow_rows(x, core), ow_send.at[1], ow_recv.at[1], (ep, left))
    ow_right.start()
    ow_left.start()
    top_half, low_half = pl.ds(0, 64), pl.ds(64, 64)
    on_right = remote(
        ow_rows(left, core).at[top_half],
        ow_rows(left, core).at[top_half],
        ow_send.at[2],
        ow_recv.at[2],
        (ep, right),
    )
    on_left = remote(
        ow_rows(right, core).at[low_half],
        ow_rows(right, core).at[low_half],
        ow_send.at[3],
        ow_recv.at[3],
        (ep, left),
    )

    def across(n, at_x):
        return remote(ow_rows(at_x, core), ow_rows(at_x, core), ow_send.at[4 + n], ow_recv.at[4 + n], partner)

    across_copies = [across(0, left), across(1, right), across(2, far)]

    @pl.when(core == 0)
    def _():
        keep_q.wait()

    @pl.when(core == 1)
    def _():
        give_q.wait_recv()

    far_q[0].wait_recv()

    depth = lax.broadcasted_iota(jnp.int32, (128, 128), 0)
    for b in range(2):
        for n in range(4):
            flipped = qb[b, pl.ds(n * 128, 128), :].astype(f32).T
            at = pl.ds(n * 128, 128)
            qt[b, 0, :, at] = jnp.where(depth < 64, flipped, 0.0).astype(bf16)
            qt[b, 1, :, at] = jnp.where(depth < 64, 0.0, flipped).astype(bf16)
    top[...] = jnp.full(top.shape, neg_big, f32)
    tot[...] = jnp.zeros(tot.shape, f32)
    acc[...] = jnp.zeros(acc.shape, f32)

    def unit(b, j, half, masked):
        for n in range(2):
            at = pl.ds(n * 256, 256)
            for m in range(2):
                q = qt[b, m, :, at]
                scores = []
                for p in range(2):
                    keys = kv[j, 2 * half + p, 0:256, :]
                    part = jnp.dot(keys, q, preferred_element_type=f32)
                    if masked:
                        key = lax.broadcasted_iota(jnp.int32, (256, 256), 0) + p * 256
                        row = lax.broadcasted_iota(jnp.int32, (256, 256), 1) + n * 256
                        part = jnp.where(key <= row, part, neg_big)
                    scores.append(part)
                old = top[b, m, :, at]
                new = old
                for part in scores:
                    new = jnp.maximum(new, jnp.max(part, axis=0, keepdims=True))
                top[b, m, :, at] = new
                fade = jnp.exp2((old - new) * scale)
                total = tot[b, m, :, at] * fade
                numer = acc[b, m, :, at] * fade
                for p in range(2):
                    exps = jnp.exp2((scores[p] - new) * scale)
                    total = total + jnp.sum(exps, axis=0, keepdims=True)
                    values = jnp.concatenate(
                        [kv[j, 2 * half + p, 256:384, :], kv[j, 2 * half + p, 384:512, :]], axis=1
                    )
                    numer = numer + jnp.dot(values, exps.astype(bf16), preferred_element_type=f32)
                tot[b, m, :, at] = total
                acc[b, m, :, at] = numer

    limits = (chip, mirror)

    def batch(items):
        def one(i, carry):
            b = lax.rem(i, 2)
            nth = i // 2
            j, half = items[0][0], jnp.int32(items[0][1])
            for k in range(1, len(items)):
                j = jnp.where(nth == k, items[k][0], j)
                half = jnp.where(nth == k, items[k][1], half)
            limit = jnp.where(b == 0, limits[0], limits[1])

            @pl.when(j < limit)
            def _():
                unit(b, j, half, False)

            return carry

        lax.fori_loop(0, 2 * len(items), one, 0)

    def arrivals(group_at, kinds):
        items = []
        for half in range(2):
            one, two = first_axis[half], 1 - first_axis[half]
            for n in group_at:
                if n == 0:
                    base, axis = (0, 0), one
                else:
                    base, axis = moved((0, 0), one, (0, -1, 1, 2)[n - 1]), two
                for by in kinds:
                    items.append((chip_at(*moved(base, axis, by)), half))
        return items

    def direct(group_at):
        for n in group_at:
            for half in range(2):
                for slot in range(2):
                    phase[half][n][slot].wait_recv()
                    phase[half][n][slot + 2].start()

    def relayed(group_at):
        for n in group_at:
            for half in range(2):
                for slot in range(2):
                    phase[half][n][slot + 2].wait_recv()

    def begin(group_at):
        for n in group_at:
            for half in range(2):
                phase[half][n][0].start()
                phase[half][n][1].start()

    unit(0, chip, 0, True)
    batch([(jnp.where(chip < mirror, chip, CHIPS), 0), (jnp.where(chip < mirror, chip, CHIPS), 1)])
    direct((0,))
    begin((2, 3))
    batch(arrivals((0,), (-1, 1)))
    relayed((0,))
    begin((4,))
    direct((1,))
    ow_right.wait_recv()
    on_right.start()
    across_copies[0].start()
    ow_left.wait_recv()
    on_left.start()
    across_copies[1].start()
    batch(arrivals((0,), (2,)) + arrivals((1,), (-1, 1)))
    direct((2, 3))
    batch(arrivals((2,), (-1, 1)) + arrivals((3,), (-1, 1)))
    relayed((1,))
    direct((4,))
    on_right.wait_recv()
    on_left.wait_recv()
    across_copies[2].start()
    batch(arrivals((1,), (2,)) + arrivals((4,), (-1, 1)))
    relayed((2, 3, 4))
    batch(arrivals((2,), (2,)) + arrivals((3,), (2,)) + arrivals((4,), (2,)))
    unit(1, mirror, 0, False)
    unit(1, mirror, 1, True)

    lam = lam_ref[core]

    def to_owner(b, n, dst):
        send = outgoing.at[b, pl.ds(n * 128, 128)]
        return remote(
            send, heads.at[2 * x + core], head_send.at[b, n], head_recv.at[2 * x + core], (dst, n)
        )

    def home(n):
        return jnp.logical_and(core == 0, x == n)

    for b in (1, 0):
        for n in range(4):
            at = pl.ds(n * 128, 128)
            head = acc[b, 0, :, at] / tot[b, 0, :, at] - lam * (acc[b, 1, :, at] / tot[b, 1, :, at])
            mean_sq = jnp.mean(head * head, axis=0, keepdims=True)
            normed = (head * lax.rsqrt(mean_sq + eps)).T * gain_ref[...]
            outgoing[b, at, :] = normed.astype(bf16)
        for n in range(4):
            if b == 0:

                @pl.when(jnp.logical_not(home(n)))
                def _(n=n):
                    to_owner(0, n, 2 * chip).start()

                @pl.when(home(n))
                def _(n=n):
                    heads[2 * x] = outgoing[0, n * 128 : (n + 1) * 128, :]

            else:
                to_owner(1, n, 2 * mirror + 1).start()

    keep_ow.wait()
    for c in across_copies:
        c.wait_recv()

    for hd in range(8):

        @pl.when(jnp.logical_or(core == 1, 2 * x != hd))
        def _(hd=hd):
            remote(heads.at[hd], heads.at[hd], head_send.at[0, 0], head_recv.at[hd], partner).wait_recv()

    def project(n, carry):
        at = pl.ds(pl.multiple_of(n * 512, 512), 512)
        total = jnp.zeros((128, 512), f32)
        for hd in range(8):
            total = total + jnp.dot(heads[hd], ow[hd, :, at], preferred_element_type=f32)
        out_ref[:, at] = total.astype(bf16)
        return carry

    lax.fori_loop(0, 4, project, 0)

    give_kv.wait_send()

    @pl.when(core == 0)
    def _():
        give_q.wait_send()

    @pl.when(core == 1)
    def _():
        far_q[0].wait_send()
        far_q[1].wait_send()

    for c in sent + [ow_right, ow_left, on_right, on_left] + across_copies:
        c.wait_send()
    for n in range(4):

        @pl.when(jnp.logical_not(home(n)))
        def _(n=n):
            to_owner(0, n, 2 * chip).wait_send()

        to_owner(1, n, 2 * mirror + 1).wait_send()


def attention(query_rows, key_rows, value_rows, lambdas, out_gain, out_weight):
    any_space = pl.BlockSpec(memory_space=pl.ANY)
    vmem = pl.BlockSpec(memory_space=pltpu.VMEM)
    width = out_weight.shape[1]
    dma = pltpu.SemaphoreType.DMA
    return pl.pallas_call(
        attention_kernel,
        out_shape=jax.ShapeDtypeStruct((128, width), bf16),
        in_specs=[any_space, vmem, vmem, pl.BlockSpec(memory_space=pltpu.SMEM), vmem, any_space],
        out_specs=vmem,
        scratch_shapes=[
            pltpu.VMEM((CHIPS, 4, 512, 128), bf16),
            pltpu.VMEM((2, 512, 128), bf16),
            pltpu.VMEM((2, 512, 128), bf16),
            pltpu.VMEM((2, 2, 128, 512), bf16),
            pltpu.VMEM((2, 2, 128, 512), f32),
            pltpu.VMEM((2, 2, 1, 512), f32),
            pltpu.VMEM((2, 2, 1, 512), f32),
            pltpu.VMEM((8, 128, width), bf16),
            pltpu.VMEM((8, 128, 128), bf16),
            pltpu.VMEM((2, 512, 128), bf16),
            dma((3,)),
            dma((3,)),
            dma((2,)),
            dma((2, 5, 4)),
            dma((2, 5, 4)),
            dma((7,)),
            dma((7,)),
            dma((2, 4)),
            dma((8,)),
        ],
        compiler_params=pltpu.CompilerParams(has_side_effects=True, vmem_limit_bytes=40 * 2**20),
        name="attention",
    )(
        query_rows,
        key_rows,
        value_rows,
        lambdas,
        out_gain.reshape(1, -1),
        out_weight.reshape(2, 128, width),
    )


def experts_part(
    tokens, norm_gain, group_ids, inner_ids, route_weights, gate_weight, up_weight, down_weight
):
    tok_dev = tokens.shape[0]
    model_width = tokens.shape[1]
    topk_count = inner_ids.shape[1]
    experts = lax.axis_size("ep")
    group_size = experts // GROUPS
    capacity = 5 * tok_dev * topk_count // (4 * experts)
    tok_wide = tokens.astype(f32)
    normed = (
        tok_wide * lax.rsqrt(jnp.mean(tok_wide * tok_wide, axis=1, keepdims=True) + eps) * norm_gain
    ).astype(bf16)
    target = (group_ids[:, None] * group_size + inner_ids).reshape(-1)
    labels = jnp.arange(experts, dtype=jnp.int32)
    onehot = (target[:, None] == labels[None, :]).astype(jnp.int32)
    slot_rank = jnp.sum((jnp.cumsum(onehot, axis=0) - 1) * onehot, axis=1)
    slot_of = target * capacity + slot_rank
    slot_ids = jnp.arange(experts * capacity, dtype=jnp.int32)
    placing = jnp.any(
        (slot_of[:, None] == slot_ids[None, :]).reshape(tok_dev, topk_count, experts * capacity),
        axis=1,
    ).astype(bf16)
    outgoing = jnp.einsum("ts,td->sd", placing, normed, preferred_element_type=f32).astype(bf16)
    arrived = lax.all_to_all(outgoing, "ep", split_axis=0, concat_axis=0, tiled=True)
    shard_rows = lax.all_gather(arrived, "tp", axis=0, tiled=True)
    gate_pre = jnp.dot(shard_rows, gate_weight[0], preferred_element_type=f32)
    up_pre = jnp.dot(shard_rows, up_weight[0], preferred_element_type=f32)
    hidden = (jax.nn.silu(gate_pre) * up_pre).astype(bf16)
    expert_term = jnp.dot(hidden, down_weight[0], preferred_element_type=f32).astype(bf16)
    results = lax.psum_scatter(expert_term, "tp", scatter_dimension=0, tiled=True)
    returned = lax.all_to_all(results, "ep", split_axis=0, concat_axis=0, tiled=True)
    picked = returned[slot_of].reshape(tok_dev, topk_count, model_width)
    return jnp.sum(picked.astype(f32) * route_weights[:, :, None], axis=1).astype(bf16)


def body(
    query_rows,
    key_rows,
    value_rows,
    lambdas,
    out_gain,
    out_weight,
    tokens,
    norm_gain,
    group_ids,
    inner_ids,
    route_weights,
    gate_weight,
    up_weight,
    down_weight,
):
    attended = attention(query_rows, key_rows, value_rows, lambdas, out_gain, out_weight)
    combined = experts_part(
        tokens, norm_gain, group_ids, inner_ids, route_weights, gate_weight, up_weight, down_weight
    )
    return (attended, combined)


def solution(mesh):
    in_specs = (
        P("ep", "tp"),
        P("ep", "tp"),
        P("ep", "tp"),
        P("tp"),
        P(),
        P("tp", None),
        P(("ep", "tp"), None),
        P(),
        P(("ep", "tp")),
        P(("ep", "tp"), None),
        P(("ep", "tp"), None),
        P("ep", None, "tp"),
        P("ep", None, "tp"),
        P("ep", "tp", None),
    )
    out_specs = (P(("ep", "tp"), None), P(("ep", "tp"), None))
    return jax.shard_map(body, mesh=mesh, in_specs=in_specs, out_specs=out_specs, check_vma=False)
```

```python
import functools
import math

import jax
import jax.numpy as jnp
from jax import lax
from jax.experimental import pallas as pl
from jax.experimental.pallas import tpu as pltpu
from jax.sharding import PartitionSpec as P

GROUPS = 4
SIDE = 4
CHIPS = 16
SLOTS = 320
ROWS = 80
BATCH = ROWS * 16
CHUNK = 160
MESH = pl.DeviceIdType.MESH

eps = 1e-06
neg_big = -1e30
f32 = jnp.float32
bf16 = jnp.bfloat16


def wrap(v):
    return lax.rem(v + SIDE, SIDE)


def layer_kernel(
    q_ref,
    k_ref,
    v_ref,
    lam_ref,
    gain_ref,
    ow_ref,
    tok_ref,
    norm_ref,
    place_ref,
    mix_ref,
    gate_ref,
    up_ref,
    down_ref,
    out_ref,
    comb_ref,
    kv,
    give,
    qb,
    qt,
    acc,
    top,
    tot,
    ow,
    heads,
    outgoing,
    pre_send,
    pre_recv,
    here,
    kv_send,
    kv_recv,
    ow_send,
    ow_recv,
    head_send,
    head_recv,
    gate_w,
    up_w,
    down_w,
    wide,
    normed_tok,
    rows_in,
    slots,
    routed,
    partial,
    far_sum,
    near_sum,
    results,
    returned,
    weights_here,
    self_here,
    out_send,
    out_recv,
    gather_send,
    gather_recv,
    far_send,
    far_recv,
    near_send,
    near_recv,
    back_send,
    back_recv,
):
    ep = lax.axis_index("ep")
    x = lax.axis_index("tp")
    chip = ep // 2
    core = lax.rem(ep, 2)
    mate = 1 - core
    mirror = CHIPS - 1 - chip
    at_z, at_y = chip // SIDE, lax.rem(chip, SIDE)
    right, left, far = wrap(x + 1), wrap(x - 1), wrap(x + 2)
    scale = (64 ** (-0.5)) * math.log2(math.e)

    def remote(src, dst, send, recv, to):
        return pltpu.make_async_remote_copy(
            src_ref=src, dst_ref=dst, send_sem=send, recv_sem=recv, device_id=to, device_id_type=MESH
        )

    def cols(head):
        return pl.ds(pl.multiple_of(head * 128, 128), 128)

    def chip_at(dz, dy):
        return wrap(at_z + dz) * SIDE + wrap(at_y + dy)

    partner = (2 * chip + mate, x)

    keep_q = pltpu.make_async_copy(q_ref.at[:, cols(0)], qb.at[0], here.at[0])
    give_q = remote(q_ref.at[:, cols(1)], qb.at[0], pre_send.at[1], pre_recv.at[1], partner)
    far_q = [
        remote(q_ref.at[:, cols(h)], qb.at[1], pre_send.at[1 + h], pre_recv.at[2], (2 * mirror + h, x))
        for h in range(2)
    ]

    @pl.when(core == 0)
    def _():
        keep_q.start()
        give_q.start()

    @pl.when(core == 1)
    def _():
        far_q[0].start()
        far_q[1].start()

    def lay_out(head, put):
        for p in range(2):
            put(p, pl.ds(0, 256), k_ref[pl.ds(p * 256, 256), cols(head)])
            for n in range(2):
                block = v_ref[pl.ds(p * 256 + n * 128, 128), cols(head)].astype(f32)
                put(p, pl.ds(256 + n * 128, 128), block.T.astype(bf16))

    def put_give(p, rows, value):
        give[p, rows, :] = value

    def put_own(p, rows, value):
        kv[chip, 2 * core + p, rows, :] = value

    lay_out(mate, put_give)
    half_of = kv.at[chip, pl.ds(2 * core, 2)]
    give_kv = remote(give, half_of, pre_send.at[0], pre_recv.at[0], partner)
    give_kv.start()
    weight_copies = [
        pltpu.make_async_copy(a, b, weights_here.at[n])
        for n, (a, b) in enumerate(((gate_ref, gate_w), (up_ref, up_w), (down_ref, down_w)))
    ]
    for c in weight_copies:
        c.start()

    tok = tok_ref[...].astype(f32)
    mean_tok = jnp.mean(tok * tok, axis=1, keepdims=True)
    normed_tok[...] = (tok * lax.rsqrt(mean_tok + eps) * norm_ref[...]).astype(bf16)
    for cb in range(16):
        wide[pl.ds(cb, SLOTS, stride=16), :] = jnp.dot(
            place_ref[...], normed_tok[:, cb * 128 : (cb + 1) * 128], preferred_element_type=f32
        )

    def to_slots(n, carry):
        at = pl.ds(pl.multiple_of(n * BATCH, BATCH), BATCH)
        slots[at, :] = wide[at, :].astype(bf16)
        return carry

    lax.fori_loop(0, 4, to_slots, 0)

    def chunk(e):
        return pl.ds(pl.multiple_of(e * CHUNK, CHUNK), CHUNK)

    def batch_rows(k):
        return pl.ds(pl.multiple_of(wrap(at_z - k) * BATCH, BATCH), BATCH)

    def plane_member(k, n):
        return chip_at(k, n // 2) * 2 + lax.rem(core + n % 2, 2)

    def dispatch(k, n):
        e = plane_member(k, n)
        return remote(
            slots.at[chunk(e)], routed.at[x, chunk(ep)], out_send.at[k, n], out_recv.at[k, n], (e, x)
        )

    pairs = [(k, n) for k in range(4) for n in range(8)]
    own_slots = pltpu.make_async_copy(slots.at[chunk(ep)], routed.at[x, chunk(ep)], self_here.at[0])
    own_slots.start()
    for k, n in pairs[1:]:
        dispatch(k, n).start()
    lay_out(core, put_own)

    def x_copy(xs, k, slot):
        at = routed.at[xs, batch_rows(k)]
        return remote(at, at, gather_send.at[k, slot], gather_recv.at[k, slot], (ep, right if slot in (0, 2) else left))

    def gather_right(k):
        return x_copy(x, k, 0)

    def gather_left(k):
        return x_copy(x, k, 1)

    def gather_relay(k):
        at = routed.at[left if k < 2 else right, batch_rows(k)]
        return remote(at, at, gather_send.at[k, 2], gather_recv.at[k, 2], (ep, right if k < 2 else left))

    def expert_term(xs, k):
        rows = pl.ds(0, BATCH)
        wide[rows, :] = routed[xs, batch_rows(k), :].astype(f32)
        for cb in range(16):
            rows_in[:, cb * 128 : (cb + 1) * 128] = wide[pl.ds(cb, ROWS, stride=16), :].astype(bf16)
        gate = jnp.dot(rows_in[...], gate_w[...], preferred_element_type=f32)
        up = jnp.dot(rows_in[...], up_w[...], preferred_element_type=f32)
        hidden = (jax.nn.silu(gate) * up).astype(bf16)
        for cb in range(8):
            part = jnp.dot(hidden, down_w[:, cb * 256 : (cb + 1) * 256], preferred_element_type=f32)
            wide[pl.ds(2 * cb, ROWS, stride=16), :] = part[:, :128]
            wide[pl.ds(2 * cb + 1, ROWS, stride=16), :] = part[:, 128:]

    def send_far(k):
        return remote(
            partial.at[2, k], far_sum.at[k], far_send.at[k], far_recv.at[k], (ep, left if k < 2 else right)
        )

    def send_left(k):
        return remote(partial.at[0, k], near_sum.at[1, k], near_send.at[0, k], near_recv.at[1, k], (ep, left))

    def send_right(k):
        return remote(partial.at[1, k], near_sum.at[0, k], near_send.at[1, k], near_recv.at[0, k], (ep, right))

    def send_back(k, n):
        e = plane_member(-k, n)
        place = 2 * wrap(at_y + n // 2) + lax.rem(core + n % 2, 2)
        return remote(
            results.at[k, chunk(place)], returned.at[chunk(ep)], back_send.at[k, n], back_recv.at[k, n], (e, x)
        )

    def step_a(k):
        for n in range(8):
            if (k, n) == (0, 0):
                own_slots.wait()
            else:
                dispatch(k, n).wait_recv()
        gather_right(k).start()
        gather_left(k).start()

    def step_b(k):
        gather_right(k).wait_recv()
        gather_left(k).wait_recv()
        gather_relay(k).start()
        if k < 2:
            expert_term(right, k)
            partial[1, k] = wide[0:BATCH, :].astype(bf16)
            send_right(k).start()
        else:
            expert_term(left, k)
            partial[0, k] = wide[0:BATCH, :].astype(bf16)
            send_left(k).start()

    def step_c(k):
        gather_relay(k).wait_recv()
        expert_term(far, k)
        partial[2, k] = wide[0:BATCH, :].astype(bf16)
        send_far(k).start()

    def step_d(k):
        side = 0 if k < 2 else 1
        expert_term(left if k < 2 else right, k)
        send_far(k).wait_recv()
        partial[side, k] = (wide[0:BATCH, :] + far_sum[k].astype(f32)).astype(bf16)
        (send_left if k < 2 else send_right)(k).start()

    def step_e(k):
        expert_term(x, k)
        send_left(k).wait_recv()
        send_right(k).wait_recv()
        results[k] = (
            wide[0:BATCH, :] + (near_sum[0, k].astype(f32) + near_sum[1, k].astype(f32))
        ).astype(bf16)
        for n in range(8):
            if (k, n) == (0, 0):
                pltpu.make_async_copy(
                    results.at[0, chunk(2 * at_y + core)], returned.at[chunk(ep)], self_here.at[1]
                ).start()
            else:
                send_back(k, n).start()

    def step_f():
        for k, n in pairs:
            if (k, n) == (0, 0):
                pltpu.make_async_copy(
                    results.at[0, chunk(2 * at_y + core)], returned.at[chunk(ep)], self_here.at[1]
                ).wait()
            else:
                send_back(k, n).wait_recv()

        def widen(n, carry):
            at = pl.ds(pl.multiple_of(n * BATCH, BATCH), BATCH)
            wide[at, :] = returned[at, :].astype(f32)
            return carry

        lax.fori_loop(0, 4, widen, 0)
        high = mix_ref[...].astype(bf16)
        low = (mix_ref[...] - high.astype(f32)).astype(bf16)
        for cb in range(16):
            got = wide[pl.ds(cb, SLOTS, stride=16), :].astype(bf16)
            total = jnp.dot(high, got, preferred_element_type=f32) + jnp.dot(
                low, got, preferred_element_type=f32
            )
            comb_ref[:, cb * 128 : (cb + 1) * 128] = total.astype(bf16)

    def step_to(axis, sign):
        return chip_at(sign, 0) if axis == 0 else chip_at(0, sign)

    def moved(place, axis, by):
        dz, dy = place
        return (dz + by, dy) if axis == 0 else (dz, dy + by)

    def spread(half, n, place, axis):
        def copy(slot):
            sign = 1 if slot % 2 == 0 else -1
            if slot < 2:
                j, part = chip_at(*place), pl.ds(2 * half, 2)
            else:
                j, part = chip_at(*moved(place, axis, -sign)), pl.ds(2 * half + slot - 2, 1)
            at = kv.at[j, part]
            return remote(
                at, at, kv_send.at[half, n, slot], kv_recv.at[half, n, slot], (2 * step_to(axis, sign) + core, x)
            )

        return [copy(slot) for slot in range(4)]

    first_axis = (1, 0)
    phase = [[None] * 5, [None] * 5]
    for half in range(2):
        one, two = first_axis[half], 1 - first_axis[half]
        phase[half][0] = spread(half, 0, (0, 0), one)
        for n, by in enumerate((0, -1, 1, 2)):
            phase[half][1 + n] = spread(half, 1 + n, moved((0, 0), one, by), two)
    sent = [c for half in range(2) for group in phase[half] for c in group]

    give_kv.wait_recv()
    for n in range(2):
        for half in range(2):
            phase[half][n][0].start()
            phase[half][n][1].start()

    keep_ow = pltpu.make_async_copy(ow_ref, ow.at[pl.ds(2 * x, 2)], here.at[1])
    keep_ow.start()

    def ow_rows(at_x, c):
        return ow.at[2 * at_x + c]

    ow_right = remote(ow_ref.at[core], ow_rows(x, core), ow_send.at[0], ow_recv.at[0], (ep, right))
    ow_left = remote(ow_ref.at[core], ow_rows(x, core), ow_send.at[1], ow_recv.at[1], (ep, left))
    ow_right.start()
    ow_left.start()
    top_half, low_half = pl.ds(0, 64), pl.ds(64, 64)
    on_right = remote(
        ow_rows(left, core).at[top_half],
        ow_rows(left, core).at[top_half],
        ow_send.at[2],
        ow_recv.at[2],
        (ep, right),
    )
    on_left = remote(
        ow_rows(right, core).at[low_half],
        ow_rows(right, core).at[low_half],
        ow_send.at[3],
        ow_recv.at[3],
        (ep, left),
    )

    def across(n, at_x):
        return remote(ow_rows(at_x, core), ow_rows(at_x, core), ow_send.at[4 + n], ow_recv.at[4 + n], partner)

    across_copies = [across(0, left), across(1, right), across(2, far)]

    @pl.when(core == 0)
    def _():
        keep_q.wait()

    @pl.when(core == 1)
    def _():
        give_q.wait_recv()

    far_q[0].wait_recv()

    depth = lax.broadcasted_iota(jnp.int32, (128, 128), 0)
    for b in range(2):
        for n in range(4):
            flipped = qb[b, pl.ds(n * 128, 128), :].astype(f32).T
            at = pl.ds(n * 128, 128)
            qt[b, 0, :, at] = jnp.where(depth < 64, flipped, 0.0).astype(bf16)
            qt[b, 1, :, at] = jnp.where(depth < 64, 0.0, flipped).astype(bf16)
    top[...] = jnp.full(top.shape, neg_big, f32)
    tot[...] = jnp.zeros(tot.shape, f32)
    acc[...] = jnp.zeros(acc.shape, f32)

    def unit(b, j, half, masked):
        for n in range(2):
            at = pl.ds(n * 256, 256)
            for m in range(2):
                q = qt[b, m, :, at]
                scores = []
                for p in range(2):
                    keys = kv[j, 2 * half + p, 0:256, :]
                    part = jnp.dot(keys, q, preferred_element_type=f32)
                    if masked:
                        key = lax.broadcasted_iota(jnp.int32, (256, 256), 0) + p * 256
                        row = lax.broadcasted_iota(jnp.int32, (256, 256), 1) + n * 256
                        part = jnp.where(key <= row, part, neg_big)
                    scores.append(part)
                old = top[b, m, :, at]
                new = old
                for part in scores:
                    new = jnp.maximum(new, jnp.max(part, axis=0, keepdims=True))
                top[b, m, :, at] = new
                fade = jnp.exp2((old - new) * scale)
                total = tot[b, m, :, at] * fade
                numer = acc[b, m, :, at] * fade
                for p in range(2):
                    exps = jnp.exp2((scores[p] - new) * scale)
                    total = total + jnp.sum(exps, axis=0, keepdims=True)
                    values = jnp.concatenate(
                        [kv[j, 2 * half + p, 256:384, :], kv[j, 2 * half + p, 384:512, :]], axis=1
                    )
                    numer = numer + jnp.dot(values, exps.astype(bf16), preferred_element_type=f32)
                tot[b, m, :, at] = total
                acc[b, m, :, at] = numer

    limits = (chip, mirror)

    def batch(items):
        def one(i, carry):
            b = lax.rem(i, 2)
            nth = i // 2
            j, half = items[0][0], jnp.int32(items[0][1])
            for k in range(1, len(items)):
                j = jnp.where(nth == k, items[k][0], j)
                half = jnp.where(nth == k, items[k][1], half)
            limit = jnp.where(b == 0, limits[0], limits[1])

            @pl.when(j < limit)
            def _():
                unit(b, j, half, False)

            return carry

        lax.fori_loop(0, 2 * len(items), one, 0)

    def arrivals(group_at, kinds):
        items = []
        for half in range(2):
            one, two = first_axis[half], 1 - first_axis[half]
            for n in group_at:
                if n == 0:
                    base, axis = (0, 0), one
                else:
                    base, axis = moved((0, 0), one, (0, -1, 1, 2)[n - 1]), two
                for by in kinds:
                    items.append((chip_at(*moved(base, axis, by)), half))
        return items

    def direct(group_at):
        for n in group_at:
            for half in range(2):
                for slot in range(2):
                    phase[half][n][slot].wait_recv()
                    phase[half][n][slot + 2].start()

    def relayed(group_at):
        for n in group_at:
            for half in range(2):
                for slot in range(2):
                    phase[half][n][slot + 2].wait_recv()

    def begin(group_at):
        for n in group_at:
            for half in range(2):
                phase[half][n][0].start()
                phase[half][n][1].start()

    for c in weight_copies:
        c.wait()
    own_late = jnp.where(chip < mirror, chip, CHIPS)
    unit(0, chip, 0, True)
    step_a(0)
    step_a(1)
    batch([(own_late, 0), (own_late, 1)])
    step_a(2)
    step_a(3)
    direct((0,))
    begin((2, 3))
    batch(arrivals((0,), (-1, 1)))
    relayed((0,))
    begin((4,))
    direct((1,))
    ow_right.wait_recv()
    on_right.start()
    across_copies[0].start()
    ow_left.wait_recv()
    on_left.start()
    across_copies[1].start()
    step_b(0)
    batch(arrivals((0,), (2,)) + arrivals((1,), (-1, 1)))
    direct((2, 3))
    step_b(1)
    batch(arrivals((2,), (-1, 1)))
    step_b(2)
    batch(arrivals((3,), (-1, 1)))
    step_b(3)
    relayed((1,))
    direct((4,))
    on_right.wait_recv()
    on_left.wait_recv()
    across_copies[2].start()
    step_c(0)
    batch(arrivals((1,), (2,)) + arrivals((4,), (-1, 1)))
    relayed((2, 3, 4))
    step_c(1)
    batch(arrivals((2,), (2,)) + arrivals((3,), (2,)) + arrivals((4,), (2,)))
    step_c(2)
    step_c(3)
    step_d(0)
    unit(1, mirror, 0, False)
    step_d(1)
    unit(1, mirror, 1, True)
    step_d(2)
    step_d(3)

    lam = lam_ref[core]

    def to_owner(b, n, dst):
        send = outgoing.at[b, pl.ds(n * 128, 128)]
        return remote(
            send, heads.at[2 * x + core], head_send.at[b, n], head_recv.at[2 * x + core], (dst, n)
        )

    def home(n):
        return jnp.logical_and(core == 0, x == n)

    for b in (1, 0):
        for n in range(4):
            at = pl.ds(n * 128, 128)
            head = acc[b, 0, :, at] / tot[b, 0, :, at] - lam * (acc[b, 1, :, at] / tot[b, 1, :, at])
            mean_sq = jnp.mean(head * head, axis=0, keepdims=True)
            normed = (head * lax.rsqrt(mean_sq + eps)).T * gain_ref[...]
            outgoing[b, at, :] = normed.astype(bf16)
        for n in range(4):
            if b == 0:

                @pl.when(jnp.logical_not(home(n)))
                def _(n=n):
                    to_owner(0, n, 2 * chip).start()

                @pl.when(home(n))
                def _(n=n):
                    heads[2 * x] = outgoing[0, n * 128 : (n + 1) * 128, :]

            else:
                to_owner(1, n, 2 * mirror + 1).start()

    for k in range(4):
        step_e(k)
    keep_ow.wait()
    for c in across_copies:
        c.wait_recv()

    for hd in range(8):

        @pl.when(jnp.logical_or(core == 1, 2 * x != hd))
        def _(hd=hd):
            remote(heads.at[hd], heads.at[hd], head_send.at[0, 0], head_recv.at[hd], partner).wait_recv()

    def project(n, carry):
        at = pl.ds(pl.multiple_of(n * 512, 512), 512)
        total = jnp.zeros((128, 512), f32)
        for hd in range(8):
            total = total + jnp.dot(heads[hd], ow[hd, :, at], preferred_element_type=f32)
        out_ref[:, at] = total.astype(bf16)
        return carry

    lax.fori_loop(0, 4, project, 0)
    step_f()

    give_kv.wait_send()

    @pl.when(core == 0)
    def _():
        give_q.wait_send()

    @pl.when(core == 1)
    def _():
        far_q[0].wait_send()
        far_q[1].wait_send()

    for c in sent + [ow_right, ow_left, on_right, on_left] + across_copies:
        c.wait_send()
    for k, n in pairs[1:]:
        dispatch(k, n).wait_send()
        send_back(k, n).wait_send()
    for k in range(4):
        for c in (gather_right(k), gather_left(k), gather_relay(k), send_far(k), send_left(k), send_right(k)):
            c.wait_send()
    for n in range(4):

        @pl.when(jnp.logical_not(home(n)))
        def _(n=n):
            to_owner(0, n, 2 * chip).wait_send()

        to_owner(1, n, 2 * mirror + 1).wait_send()


def layer(query_rows, key_rows, value_rows, lambdas, out_gain, out_weight, tokens, norm_gain, place, mix, weights):
    any_space = pl.BlockSpec(memory_space=pl.ANY)
    vmem = pl.BlockSpec(memory_space=pltpu.VMEM)
    width = out_weight.shape[1]
    dma = pltpu.SemaphoreType.DMA
    shape = jax.ShapeDtypeStruct((128, width), bf16)
    return pl.pallas_call(
        layer_kernel,
        out_shape=(shape, shape),
        in_specs=[any_space, vmem, vmem, pl.BlockSpec(memory_space=pltpu.SMEM), vmem, any_space]
        + [vmem] * 4
        + [any_space] * 3,
        out_specs=(vmem, vmem),
        scratch_shapes=[
            pltpu.VMEM((CHIPS, 4, 512, 128), bf16),
            pltpu.VMEM((2, 512, 128), bf16),
            pltpu.VMEM((2, 512, 128), bf16),
            pltpu.VMEM((2, 2, 128, 512), bf16),
            pltpu.VMEM((2, 2, 128, 512), f32),
            pltpu.VMEM((2, 2, 1, 512), f32),
            pltpu.VMEM((2, 2, 1, 512), f32),
            pltpu.VMEM((8, 128, width), bf16),
            pltpu.VMEM((8, 128, 128), bf16),
            pltpu.VMEM((2, 512, 128), bf16),
            dma((3,)),
            dma((3,)),
            dma((2,)),
            dma((2, 5, 4)),
            dma((2, 5, 4)),
            dma((7,)),
            dma((7,)),
            dma((2, 4)),
            dma((8,)),
            pltpu.VMEM((width, 256), bf16),
            pltpu.VMEM((width, 256), bf16),
            pltpu.VMEM((256, width), bf16),
            pltpu.VMEM((4 * BATCH, 128), f32),
            pltpu.VMEM((128, width), bf16),
            pltpu.VMEM((ROWS, width), bf16),
            pltpu.VMEM((4 * BATCH, 128), bf16),
            pltpu.VMEM((4, 4 * BATCH, 128), bf16),
            pltpu.VMEM((3, 4, BATCH, 128), bf16),
            pltpu.VMEM((4, BATCH, 128), bf16),
            pltpu.VMEM((2, 4, BATCH, 128), bf16),
            pltpu.VMEM((4, BATCH, 128), bf16),
            pltpu.VMEM((4 * BATCH, 128), bf16),
            dma((3,)),
            dma((2,)),
            dma((4, 8)),
            dma((4, 8)),
            dma((4, 3)),
            dma((4, 3)),
            dma((4,)),
            dma((4,)),
            dma((2, 4)),
            dma((2, 4)),
            dma((4, 8)),
            dma((4, 8)),
        ],
        compiler_params=pltpu.CompilerParams(has_side_effects=True, vmem_limit_bytes=60 * 2**20),
        name="layer",
    )(
        query_rows,
        key_rows,
        value_rows,
        lambdas,
        out_gain.reshape(1, -1),
        out_weight.reshape(2, 128, width),
        tokens,
        norm_gain.reshape(1, -1),
        place,
        mix,
        *weights,
    )


def routing(group_ids, inner_ids, route_weights):
    tok_dev, topk_count = inner_ids.shape
    experts = lax.axis_size("ep")
    group_size = experts // GROUPS
    capacity = 5 * tok_dev * topk_count // (4 * experts)
    target = (group_ids[:, None] * group_size + inner_ids).reshape(-1)
    labels = jnp.arange(experts, dtype=jnp.int32)
    onehot = (target[:, None] == labels[None, :]).astype(jnp.int32)
    slot_rank = jnp.sum((jnp.cumsum(onehot, axis=0) - 1) * onehot, axis=1)
    slot_of = (target * capacity + slot_rank).reshape(tok_dev, topk_count)
    slot_ids = jnp.arange(experts * capacity, dtype=jnp.int32)
    place = jnp.any(slot_ids[:, None, None] == slot_of[None], axis=2).astype(bf16)
    chosen = slot_of[:, :, None] == slot_ids[None, None, :]
    mix = jnp.sum(jnp.where(chosen, route_weights[:, :, None], 0.0), axis=1)
    return place, mix


def body(
    query_rows,
    key_rows,
    value_rows,
    lambdas,
    out_gain,
    out_weight,
    tokens,
    norm_gain,
    group_ids,
    inner_ids,
    route_weights,
    gate_weight,
    up_weight,
    down_weight,
):
    place, mix = routing(group_ids, inner_ids, route_weights)
    return layer(
        query_rows,
        key_rows,
        value_rows,
        lambdas,
        out_gain,
        out_weight,
        tokens,
        norm_gain,
        place,
        mix,
        (gate_weight[0], up_weight[0], down_weight[0]),
    )


def solution(mesh):
    in_specs = (
        P("ep", "tp"),
        P("ep", "tp"),
        P("ep", "tp"),
        P("tp"),
        P(),
        P("tp", None),
        P(("ep", "tp"), None),
        P(),
        P(("ep", "tp")),
        P(("ep", "tp"), None),
        P(("ep", "tp"), None),
        P("ep", None, "tp"),
        P("ep", None, "tp"),
        P("ep", "tp", None),
    )
    out_specs = (P(("ep", "tp"), None), P(("ep", "tp"), None))
    return jax.shard_map(body, mesh=mesh, in_specs=in_specs, out_specs=out_specs, check_vma=False)
```

```python
import functools
import math

import jax
import jax.numpy as jnp
from jax import lax
from jax.experimental import pallas as pl
from jax.experimental.pallas import tpu as pltpu
from jax.sharding import PartitionSpec as P

GROUPS = 4
SIDE = 4
CHIPS = 16
SLOTS = 320
ROWS = 80
BATCH = ROWS * 16
CHUNK = 160
MESH = pl.DeviceIdType.MESH

eps = 1e-06
neg_big = -1e30
f32 = jnp.float32
bf16 = jnp.bfloat16


def wrap(v):
    return lax.rem(v + SIDE, SIDE)


def layer_kernel(
    q_ref,
    k_ref,
    v_ref,
    lam_ref,
    gain_ref,
    ow_ref,
    tok_ref,
    norm_ref,
    place_ref,
    mix_ref,
    gate_ref,
    up_ref,
    down_ref,
    out_ref,
    comb_ref,
    kv,
    give,
    qb,
    qt,
    acc,
    top,
    tot,
    ow,
    ow_mate,
    heads,
    outgoing,
    pre_send,
    pre_recv,
    here,
    kv_send,
    kv_recv,
    ow_send,
    ow_recv,
    head_send,
    head_recv,
    gate_w,
    up_w,
    down_w,
    wide,
    normed_tok,
    rows_in,
    slots,
    routed,
    partial,
    far_sum,
    near_sum,
    results,
    returned,
    weights_here,
    self_here,
    out_send,
    out_recv,
    gather_send,
    gather_recv,
    far_send,
    far_recv,
    near_send,
    near_recv,
    back_send,
    back_recv,
):
    ep = lax.axis_index("ep")
    x = lax.axis_index("tp")
    chip = ep // 2
    core = lax.rem(ep, 2)
    mate = 1 - core
    mirror = CHIPS - 1 - chip
    at_z, at_y = chip // SIDE, lax.rem(chip, SIDE)
    right, left, far = wrap(x + 1), wrap(x - 1), wrap(x + 2)
    scale = (64 ** (-0.5)) * math.log2(math.e)

    def remote(src, dst, send, recv, to):
        return pltpu.make_async_remote_copy(
            src_ref=src, dst_ref=dst, send_sem=send, recv_sem=recv, device_id=to, device_id_type=MESH
        )

    def cols(head):
        return pl.ds(pl.multiple_of(head * 128, 128), 128)

    def chip_at(dz, dy):
        return wrap(at_z + dz) * SIDE + wrap(at_y + dy)

    partner = (2 * chip + mate, x)

    barrier = pltpu.get_barrier_semaphore()

    def greet(e, at_x):
        pl.semaphore_signal(barrier, inc=1, device_id=(e, at_x), device_id_type=MESH)

    def greet_all(n, carry):
        greet(lax.rem(ep + n, 2 * CHIPS), x)
        return carry

    lax.fori_loop(1, 2 * CHIPS, greet_all, 0)
    for d in range(1, SIDE):
        for e in (ep, 2 * chip + mate, 2 * mirror, 2 * mirror + 1):
            greet(e, wrap(x + d))

    weight_copies = [
        pltpu.make_async_copy(a, b, weights_here.at[n])
        for n, (a, b) in enumerate(((gate_ref, gate_w), (up_ref, up_w), (down_ref, down_w)))
    ]
    for c in weight_copies:
        c.start()

    tok = tok_ref[...].astype(f32)
    mean_tok = jnp.mean(tok * tok, axis=1, keepdims=True)
    normed_tok[...] = (tok * lax.rsqrt(mean_tok + eps) * norm_ref[...]).astype(bf16)
    for cb in range(16):
        wide[pl.ds(cb, SLOTS, stride=16), :] = jnp.dot(
            place_ref[...], normed_tok[:, cb * 128 : (cb + 1) * 128], preferred_element_type=f32
        )

    def to_slots(n, carry):
        at = pl.ds(pl.multiple_of(n * BATCH, BATCH), BATCH)
        slots[at, :] = wide[at, :].astype(bf16)
        return carry

    lax.fori_loop(0, 4, to_slots, 0)

    def chunk(e):
        return pl.ds(pl.multiple_of(e * CHUNK, CHUNK), CHUNK)

    def batch_rows(k):
        return pl.ds(pl.multiple_of(wrap(at_z - k) * BATCH, BATCH), BATCH)

    def plane_member(k, n):
        return chip_at(k, n // 2) * 2 + lax.rem(core + n % 2, 2)

    def dispatch(k, n):
        e = plane_member(k, n)
        return remote(
            slots.at[chunk(e)], routed.at[x, chunk(ep)], out_send.at[k, n], out_recv.at[k, n], (e, x)
        )

    pairs = [(k, n) for k in range(4) for n in range(8)]
    own_slots = pltpu.make_async_copy(slots.at[chunk(ep)], routed.at[x, chunk(ep)], self_here.at[0])
    own_slots.start()
    pl.semaphore_wait(barrier, 2 * CHIPS - 1 + 4 * (SIDE - 1))

    def dispatch_plane(k):
        for n in range(8):
            if (k, n) != (0, 0):
                dispatch(k, n).start()

    dispatch_plane(0)

    keep_q = pltpu.make_async_copy(q_ref.at[:, cols(0)], qb.at[0], here.at[0])
    give_q = remote(q_ref.at[:, cols(1)], qb.at[0], pre_send.at[1], pre_recv.at[1], partner)
    far_q = [
        remote(q_ref.at[:, cols(h)], qb.at[1], pre_send.at[1 + h], pre_recv.at[2], (2 * mirror + h, x))
        for h in range(2)
    ]

    @pl.when(core == 0)
    def _():
        keep_q.start()
        give_q.start()

    @pl.when(core == 1)
    def _():
        far_q[0].start()
        far_q[1].start()

    def lay_out(head, put):
        for p in range(2):
            put(p, pl.ds(0, 256), k_ref[pl.ds(p * 256, 256), cols(head)])
            for n in range(2):
                block = v_ref[pl.ds(p * 256 + n * 128, 128), cols(head)].astype(f32)
                put(p, pl.ds(256 + n * 128, 128), block.T.astype(bf16))

    def put_give(p, rows, value):
        give[p, rows, :] = value

    def put_own(p, rows, value):
        kv[chip, 2 * core + p, rows, :] = value

    lay_out(mate, put_give)
    half_of = kv.at[chip, pl.ds(2 * core, 2), pl.ds(0, 512)]
    give_kv = remote(give, half_of, pre_send.at[0], pre_recv.at[0], partner)
    give_kv.start()
    dispatch_plane(1)
    lay_out(core, put_own)

    def x_copy(xs, k, slot):
        at = routed.at[xs, batch_rows(k)]
        return remote(at, at, gather_send.at[k, slot], gather_recv.at[k, slot], (ep, right if slot in (0, 2) else left))

    def gather_right(k):
        return x_copy(x, k, 0)

    def gather_left(k):
        return x_copy(x, k, 1)

    def gather_relay(k):
        at = routed.at[left if k < 2 else right, batch_rows(k)]
        return remote(at, at, gather_send.at[k, 2], gather_recv.at[k, 2], (ep, right if k < 2 else left))

    def expert_term(xs, k):
        rows = pl.ds(0, BATCH)
        wide[rows, :] = routed[xs, batch_rows(k), :].astype(f32)
        for cb in range(16):
            rows_in[:, cb * 128 : (cb + 1) * 128] = wide[pl.ds(cb, ROWS, stride=16), :].astype(bf16)
        gate = jnp.dot(rows_in[...], gate_w[...], preferred_element_type=f32)
        up = jnp.dot(rows_in[...], up_w[...], preferred_element_type=f32)
        hidden = (jax.nn.silu(gate) * up).astype(bf16)
        for cb in range(8):
            part = jnp.dot(hidden, down_w[:, cb * 256 : (cb + 1) * 256], preferred_element_type=f32)
            wide[pl.ds(2 * cb, ROWS, stride=16), :] = part[:, :128]
            wide[pl.ds(2 * cb + 1, ROWS, stride=16), :] = part[:, 128:]

    def send_far(k):
        return remote(
            partial.at[2, k], far_sum.at[k], far_send.at[k], far_recv.at[k], (ep, left if k < 2 else right)
        )

    def send_left(k):
        return remote(partial.at[0, k], near_sum.at[1, k], near_send.at[0, k], near_recv.at[1, k], (ep, left))

    def send_right(k):
        return remote(partial.at[1, k], near_sum.at[0, k], near_send.at[1, k], near_recv.at[0, k], (ep, right))

    def send_back(k, n):
        e = plane_member(-k, n)
        place = 2 * wrap(at_y + n // 2) + lax.rem(core + n % 2, 2)
        return remote(
            results.at[k, chunk(place)], returned.at[chunk(ep)], back_send.at[k, n], back_recv.at[k, n], (e, x)
        )

    def step_a(k):
        for n in range(8):
            if (k, n) == (0, 0):
                own_slots.wait()
            else:
                dispatch(k, n).wait_recv()
        gather_right(k).start()
        gather_left(k).start()

    def step_b(k):
        gather_right(k).wait_recv()
        gather_left(k).wait_recv()
        gather_relay(k).start()

    def step_near(k):
        if k < 2:
            expert_term(right, k)
            partial[1, k] = wide[0:BATCH, :].astype(bf16)
            send_right(k).start()
        else:
            expert_term(left, k)
            partial[0, k] = wide[0:BATCH, :].astype(bf16)
            send_left(k).start()

    def step_c(k):
        gather_relay(k).wait_recv()
        expert_term(far, k)
        partial[2, k] = wide[0:BATCH, :].astype(bf16)
        send_far(k).start()

    def step_d(k):
        side = 0 if k < 2 else 1
        expert_term(left if k < 2 else right, k)
        send_far(k).wait_recv()
        partial[side, k] = (wide[0:BATCH, :] + far_sum[k].astype(f32)).astype(bf16)
        (send_left if k < 2 else send_right)(k).start()

    def step_e(k):
        expert_term(x, k)
        send_left(k).wait_recv()
        send_right(k).wait_recv()
        results[k] = (
            wide[0:BATCH, :] + (near_sum[0, k].astype(f32) + near_sum[1, k].astype(f32))
        ).astype(bf16)
        for n in range(8):
            if (k, n) == (0, 0):
                pltpu.make_async_copy(
                    results.at[0, chunk(2 * at_y + core)], returned.at[chunk(ep)], self_here.at[1]
                ).start()
            else:
                send_back(k, n).start()

    def step_f():
        for k, n in pairs:
            if (k, n) == (0, 0):
                pltpu.make_async_copy(
                    results.at[0, chunk(2 * at_y + core)], returned.at[chunk(ep)], self_here.at[1]
                ).wait()
            else:
                send_back(k, n).wait_recv()

        def widen(n, carry):
            at = pl.ds(pl.multiple_of(n * BATCH, BATCH), BATCH)
            wide[at, :] = returned[at, :].astype(f32)
            return carry

        lax.fori_loop(0, 4, widen, 0)
        high = mix_ref[...].astype(bf16)
        low = (mix_ref[...] - high.astype(f32)).astype(bf16)
        for cb in range(16):
            got = wide[pl.ds(cb, SLOTS, stride=16), :].astype(bf16)
            total = jnp.dot(high, got, preferred_element_type=f32) + jnp.dot(
                low, got, preferred_element_type=f32
            )
            comb_ref[:, cb * 128 : (cb + 1) * 128] = total.astype(bf16)

    def step_to(axis, sign):
        return chip_at(sign, 0) if axis == 0 else chip_at(0, sign)

    def moved(place, axis, by):
        dz, dy = place
        return (dz + by, dy) if axis == 0 else (dz, dy + by)

    def spread(half, n, place, axis):
        def copy(slot):
            sign = 1 if slot % 2 == 0 else -1
            if slot < 2:
                j, part = chip_at(*place), pl.ds(2 * half, 2)
            else:
                j, part = chip_at(*moved(place, axis, -sign)), pl.ds(2 * half + slot - 2, 1)
            at = kv.at[j, part]
            return remote(
                at, at, kv_send.at[half, n, slot], kv_recv.at[half, n, slot], (2 * step_to(axis, sign) + core, x)
            )

        return [copy(slot) for slot in range(4)]

    first_axis = (1, 0)
    phase = [[None] * 5, [None] * 5]
    for half in range(2):
        one, two = first_axis[half], 1 - first_axis[half]
        phase[half][0] = spread(half, 0, (0, 0), one)
        for n, by in enumerate((0, -1, 1, 2)):
            phase[half][1 + n] = spread(half, 1 + n, moved((0, 0), one, by), two)
    sent = [c for half in range(2) for group in phase[half] for c in group]

    keep_ow = pltpu.make_async_copy(ow_ref, ow, here.at[1])
    keep_ow.start()

    def ow_copy(d):
        return remote(
            ow_ref.at[core, :, cols(chip)],
            kv.at[chip, 3 - d, pl.ds(512, 128)],
            ow_send.at[d - 1],
            ow_recv.at[3 - d],
            (ep, wrap(x + d)),
        )

    ow_copies = [ow_copy(d) for d in (1, 2, 3)]
    for c in ow_copies:
        c.start()
    kv[chip, 3, pl.ds(512, 128), :] = jnp.zeros((128, 128), bf16)
    across = remote(
        kv.at[:, pl.ds(0, 3), pl.ds(512, 128)], ow_mate, ow_send.at[3], ow_recv.at[3], partner
    )

    @pl.when(core == 0)
    def _():
        keep_q.wait()

    @pl.when(core == 1)
    def _():
        give_q.wait_recv()

    far_q[0].wait_recv()

    depth = lax.broadcasted_iota(jnp.int32, (128, 128), 0)
    for b in range(2):
        for n in range(4):
            flipped = qb[b, pl.ds(n * 128, 128), :].astype(f32).T
            at = pl.ds(n * 128, 128)
            qt[b, 0, :, at] = jnp.where(depth < 64, flipped, 0.0).astype(bf16)
            qt[b, 1, :, at] = jnp.where(depth < 64, 0.0, flipped).astype(bf16)
    top[...] = jnp.full(top.shape, neg_big, f32)
    tot[...] = jnp.zeros(tot.shape, f32)
    acc[...] = jnp.zeros(acc.shape, f32)

    def unit(b, j, half, masked):
        for n in range(2):
            at = pl.ds(n * 256, 256)
            for m in range(2):
                q = qt[b, m, :, at]
                scores = []
                for p in range(2):
                    keys = kv[j, 2 * half + p, 0:256, :]
                    part = jnp.dot(keys, q, preferred_element_type=f32)
                    if masked:
                        key = lax.broadcasted_iota(jnp.int32, (256, 256), 0) + p * 256
                        row = lax.broadcasted_iota(jnp.int32, (256, 256), 1) + n * 256
                        part = jnp.where(key <= row, part, neg_big)
                    scores.append(part)
                old = top[b, m, :, at]
                new = old
                for part in scores:
                    new = jnp.maximum(new, jnp.max(part, axis=0, keepdims=True))
                top[b, m, :, at] = new
                fade = jnp.exp2((old - new) * scale)
                total = tot[b, m, :, at] * fade
                numer = acc[b, m, :, at] * fade
                for p in range(2):
                    exps = jnp.exp2((scores[p] - new) * scale)
                    total = total + jnp.sum(exps, axis=0, keepdims=True)
                    values = jnp.concatenate(
                        [kv[j, 2 * half + p, 256:384, :], kv[j, 2 * half + p, 384:512, :]], axis=1
                    )
                    numer = numer + jnp.dot(values, exps.astype(bf16), preferred_element_type=f32)
                tot[b, m, :, at] = total
                acc[b, m, :, at] = numer

    limits = (chip, mirror)

    def batch(items):
        def one(i, carry):
            b = lax.rem(i, 2)
            nth = i // 2
            j, half = items[0][0], jnp.int32(items[0][1])
            for k in range(1, len(items)):
                j = jnp.where(nth == k, items[k][0], j)
                half = jnp.where(nth == k, items[k][1], half)
            limit = jnp.where(b == 0, limits[0], limits[1])

            @pl.when(j < limit)
            def _():
                unit(b, j, half, False)

            return carry

        lax.fori_loop(0, 2 * len(items), one, 0)

    def arrivals(group_at, kinds):
        items = []
        for half in range(2):
            one, two = first_axis[half], 1 - first_axis[half]
            for n in group_at:
                if n == 0:
                    base, axis = (0, 0), one
                else:
                    base, axis = moved((0, 0), one, (0, -1, 1, 2)[n - 1]), two
                for by in kinds:
                    items.append((chip_at(*moved(base, axis, by)), half))
        return items

    def direct(group_at):
        for n in group_at:
            for half in range(2):
                for slot in range(2):
                    phase[half][n][slot].wait_recv()
                    phase[half][n][slot + 2].start()

    def relayed(group_at):
        for n in group_at:
            for half in range(2):
                for slot in range(2):
                    phase[half][n][slot + 2].wait_recv()

    def begin(group_at):
        for n in group_at:
            for half in range(2):
                phase[half][n][0].start()
                phase[half][n][1].start()

    for c in weight_copies:
        c.wait()
    own_late = jnp.where(chip < mirror, chip, CHIPS)
    step_a(0)
    dispatch_plane(2)
    give_kv.wait_recv()
    unit(0, chip, 0, True)
    step_a(1)
    dispatch_plane(3)
    for c in ow_copies:
        c.wait_recv()
    step_a(2)
    begin((0, 1))
    step_a(3)
    batch([(own_late, 0), (own_late, 1)])
    direct((0,))
    begin((2, 3))
    step_b(0)
    batch(arrivals((0,), (-1, 1)))
    step_b(1)
    relayed((0,))
    begin((4,))
    direct((1,))
    batch(arrivals((0,), (2,)))
    step_b(2)
    batch(arrivals((1,), (-1, 1)))
    step_b(3)
    direct((2, 3))
    step_c(0)
    batch(arrivals((2,), (-1, 1)))
    step_c(2)
    step_c(1)
    batch(arrivals((3,), (-1, 1)))
    step_c(3)
    step_near(0)
    step_near(2)
    relayed((1,))
    direct((4,))
    step_d(0)
    step_d(2)
    batch(arrivals((1,), (2,)) + arrivals((4,), (-1, 1)))
    step_near(1)
    step_near(3)
    relayed((2, 3, 4))
    across.start()
    step_d(1)
    step_d(3)
    batch(arrivals((2,), (2,)) + arrivals((3,), (2,)) + arrivals((4,), (2,)))
    step_e(0)
    step_e(2)
    unit(1, mirror, 0, False)
    unit(1, mirror, 1, True)

    lam = lam_ref[core]

    def to_owner(b, n, dst):
        send = outgoing.at[b, pl.ds(n * 128, 128)]
        return remote(
            send, heads.at[2 * x + core], head_send.at[b, n], head_recv.at[2 * x + core], (dst, n)
        )

    def home(n):
        return jnp.logical_and(core == 0, x == n)

    for b in (1, 0):
        for n in range(4):
            at = pl.ds(n * 128, 128)
            head = acc[b, 0, :, at] / tot[b, 0, :, at] - lam * (acc[b, 1, :, at] / tot[b, 1, :, at])
            mean_sq = jnp.mean(head * head, axis=0, keepdims=True)
            normed = (head * lax.rsqrt(mean_sq + eps)).T * gain_ref[...]
            outgoing[b, at, :] = normed.astype(bf16)
        for n in range(4):
            if b == 0:

                @pl.when(jnp.logical_not(home(n)))
                def _(n=n):
                    to_owner(0, n, 2 * chip).start()

                @pl.when(home(n))
                def _(n=n):
                    heads[2 * x] = outgoing[0, n * 128 : (n + 1) * 128, :]

            else:
                to_owner(1, n, 2 * mirror + 1).start()

    step_e(1)
    step_e(3)
    keep_ow.wait()
    across.wait_recv()

    for hd in range(8):

        @pl.when(jnp.logical_or(core == 1, 2 * x != hd))
        def _(hd=hd):
            remote(heads.at[hd], heads.at[hd], head_send.at[0, 0], head_recv.at[hd], partner).wait_recv()

    def project(j, carry):
        at = cols(j)
        total = jnp.zeros((128, 128), f32)
        for n in range(2):
            total = total + jnp.dot(heads[2 * x + n], ow[n, :, at], preferred_element_type=f32)
        for p in range(3):
            other = 2 * wrap(x + 1 + p)
            total = total + jnp.dot(heads[other + core], kv[j, p, 512:640, :], preferred_element_type=f32)
            total = total + jnp.dot(heads[other + mate], ow_mate[j, p], preferred_element_type=f32)
        out_ref[:, at] = total.astype(bf16)
        return carry

    lax.fori_loop(0, CHIPS, project, 0)
    step_f()

    give_kv.wait_send()

    @pl.when(core == 0)
    def _():
        give_q.wait_send()

    @pl.when(core == 1)
    def _():
        far_q[0].wait_send()
        far_q[1].wait_send()

    for c in sent + ow_copies + [across]:
        c.wait_send()
    for k, n in pairs[1:]:
        dispatch(k, n).wait_send()
        send_back(k, n).wait_send()
    for k in range(4):
        for c in (gather_right(k), gather_left(k), gather_relay(k), send_far(k), send_left(k), send_right(k)):
            c.wait_send()
    for n in range(4):

        @pl.when(jnp.logical_not(home(n)))
        def _(n=n):
            to_owner(0, n, 2 * chip).wait_send()

        to_owner(1, n, 2 * mirror + 1).wait_send()


def layer(query_rows, key_rows, value_rows, lambdas, out_gain, out_weight, tokens, norm_gain, place, mix, weights):
    any_space = pl.BlockSpec(memory_space=pl.ANY)
    vmem = pl.BlockSpec(memory_space=pltpu.VMEM)
    width = out_weight.shape[1]
    dma = pltpu.SemaphoreType.DMA
    shape = jax.ShapeDtypeStruct((128, width), bf16)
    return pl.pallas_call(
        layer_kernel,
        out_shape=(shape, shape),
        in_specs=[any_space, vmem, vmem, pl.BlockSpec(memory_space=pltpu.SMEM), vmem, any_space]
        + [vmem] * 4
        + [any_space] * 3,
        out_specs=(vmem, vmem),
        scratch_shapes=[
            pltpu.VMEM((CHIPS, 4, 640, 128), bf16),
            pltpu.VMEM((2, 512, 128), bf16),
            pltpu.VMEM((2, 512, 128), bf16),
            pltpu.VMEM((2, 2, 128, 512), bf16),
            pltpu.VMEM((2, 2, 128, 512), f32),
            pltpu.VMEM((2, 2, 1, 512), f32),
            pltpu.VMEM((2, 2, 1, 512), f32),
            pltpu.VMEM((2, 128, width), bf16),
            pltpu.VMEM((CHIPS, 3, 128, 128), bf16),
            pltpu.VMEM((8, 128, 128), bf16),
            pltpu.VMEM((2, 512, 128), bf16),
            dma((3,)),
            dma((3,)),
            dma((2,)),
            dma((2, 5, 4)),
            dma((2, 5, 4)),
            dma((4,)),
            dma((4,)),
            dma((2, 4)),
            dma((8,)),
            pltpu.VMEM((width, 256), bf16),
            pltpu.VMEM((width, 256), bf16),
            pltpu.VMEM((256, width), bf16),
            pltpu.VMEM((4 * BATCH, 128), f32),
            pltpu.VMEM((128, width), bf16),
            pltpu.VMEM((ROWS, width), bf16),
            pltpu.VMEM((4 * BATCH, 128), bf16),
            pltpu.VMEM((4, 4 * BATCH, 128), bf16),
            pltpu.VMEM((3, 4, BATCH, 128), bf16),
            pltpu.VMEM((4, BATCH, 128), bf16),
            pltpu.VMEM((2, 4, BATCH, 128), bf16),
            pltpu.VMEM((4, BATCH, 128), bf16),
            pltpu.VMEM((4 * BATCH, 128), bf16),
            dma((3,)),
            dma((2,)),
            dma((4, 8)),
            dma((4, 8)),
            dma((4, 3)),
            dma((4, 3)),
            dma((4,)),
            dma((4,)),
            dma((2, 4)),
            dma((2, 4)),
            dma((4, 8)),
            dma((4, 8)),
        ],
        compiler_params=pltpu.CompilerParams(collective_id=0, has_side_effects=True, vmem_limit_bytes=60 * 2**20),
        name="layer",
    )(
        query_rows,
        key_rows,
        value_rows,
        lambdas,
        out_gain.reshape(1, -1),
        out_weight.reshape(2, 128, width),
        tokens,
        norm_gain.reshape(1, -1),
        place,
        mix,
        *weights,
    )


def routing(group_ids, inner_ids, route_weights):
    tok_dev, topk_count = inner_ids.shape
    experts = lax.axis_size("ep")
    group_size = experts // GROUPS
    capacity = 5 * tok_dev * topk_count // (4 * experts)
    target = (group_ids[:, None] * group_size + inner_ids).reshape(-1)
    labels = jnp.arange(experts, dtype=jnp.int32)
    onehot = (target[:, None] == labels[None, :]).astype(jnp.int32)
    slot_rank = jnp.sum((jnp.cumsum(onehot, axis=0) - 1) * onehot, axis=1)
    slot_of = (target * capacity + slot_rank).reshape(tok_dev, topk_count)
    slot_ids = jnp.arange(experts * capacity, dtype=jnp.int32)
    place = jnp.any(slot_ids[:, None, None] == slot_of[None], axis=2).astype(bf16)
    chosen = slot_of[:, :, None] == slot_ids[None, None, :]
    mix = jnp.sum(jnp.where(chosen, route_weights[:, :, None], 0.0), axis=1)
    return place, mix


def body(
    query_rows,
    key_rows,
    value_rows,
    lambdas,
    out_gain,
    out_weight,
    tokens,
    norm_gain,
    group_ids,
    inner_ids,
    route_weights,
    gate_weight,
    up_weight,
    down_weight,
):
    place, mix = routing(group_ids, inner_ids, route_weights)
    return layer(
        query_rows,
        key_rows,
        value_rows,
        lambdas,
        out_gain,
        out_weight,
        tokens,
        norm_gain,
        place,
        mix,
        (gate_weight[0], up_weight[0], down_weight[0]),
    )


def solution(mesh):
    in_specs = (
        P("ep", "tp"),
        P("ep", "tp"),
        P("ep", "tp"),
        P("tp"),
        P(),
        P("tp", None),
        P(("ep", "tp"), None),
        P(),
        P(("ep", "tp")),
        P(("ep", "tp"), None),
        P(("ep", "tp"), None),
        P("ep", None, "tp"),
        P("ep", None, "tp"),
        P("ep", "tp", None),
    )
    out_specs = (P(("ep", "tp"), None), P(("ep", "tp"), None))
    return jax.shard_map(body, mesh=mesh, in_specs=in_specs, out_specs=out_specs, check_vma=False)
```
